32 devices in a mesh: kv: 8 (over z, y), tp: 4 (over x, core).
Axes of the slice: x: 2, y: 2, z: 4, core: 2. Of those that a mesh axis runs over, the one named last changes fastest.
Arguments:
- hidden_rows: bfloat16 [8192, 4096], P(('kv', 'tp')), may hold values from -6 to 6
- queries: bfloat16 [8192, 4096], P('kv', 'tp'), may hold values from -6 to 6
- key_rows: bfloat16 [8192, 1024], P('kv', 'tp'), may hold values from -6 to 6
- value_rows: bfloat16 [8192, 1024], P('kv', 'tp'), may hold values from -6 to 6
- branch_gates: float32 [2, 32, 8192], P(None, 'tp', 'kv'), may hold values from 0.05 to 0.95
- log_sums: float32 [2, 32, 8192], P(None, 'tp', 'kv'), may hold values from 1 to 7
- chosen: int32 [8, 64, 16], P('tp', 'kv'), may hold values from 0 to 255, as said below
- out_grad: bfloat16 [8192, 4096], P('kv', 'tp'), may hold values from -6 to 6
Outputs:
- grad_queries: bfloat16 [8192, 4096], P('kv', 'tp')
- grad_keys: bfloat16 [8192, 1024], P('kv', 'tp')
- grad_values: bfloat16 [8192, 1024], P('kv', 'tp')
- grad_weight: float32 [4096, 4096], P('kv', 'tp')
The draws below stay inside these ranges and needn't reach their ends.
Inputs may be any that keep to these rules, and one draw needn't show every extreme that they name: `chosen`: each list names distinct key blocks, among them the blocks that cover the query block's own rows; blocks past a query's position may be named and carry no weight for it. For one key head, the lists of the query blocks of one index of kv name at most 16 key blocks (counted with repetition) that lie at any one other index of kv.
All inputs are finite; a program needn't handle non-finite values.
Results may differ from the reference program's by a relative error of at most 0.011.
Values may be sent and summed in bfloat16 or wider, within the bound.
A program may use at most 128 MiB of HBM per device.

```python
import jax
import jax.numpy as jnp
from jax import lax

MODEL = 4096
HEADS = 32
KV_HEADS = 8
HEAD_DIM = 128
TOK_DEV = 1024
QUERY_BLOCK = 128
KEY_BLOCK = 32
POOL_BLOCK = 32
CHOSEN = 16
SEQ = 8192


def block_shared_rows(key):
    width = KV_HEADS * HEAD_DIM
    pool_count = SEQ // POOL_BLOCK
    key_parts = jax.random.split(key, 2)
    common = 0.8 * jax.random.normal(key_parts[0], (pool_count, 1, width), jnp.float32)
    rough = 0.6 * jax.random.normal(key_parts[1], (pool_count, POOL_BLOCK, width), jnp.float32)
    rows = jnp.clip((common + rough).reshape(SEQ, width), -6.0, 6.0)
    return rows.astype(jnp.bfloat16)


def draw_key_rows(key, part):
    return block_shared_rows(jax.random.fold_in(key, 31))


def draw_value_rows(key, part):
    return block_shared_rows(jax.random.fold_in(key, 37))


def draw_log_sums(key, part):
    key_parts = jax.random.split(jax.random.fold_in(key, 17), 2)
    seen_count = (jnp.arange(SEQ, dtype=jnp.int32) + 1) // POOL_BLOCK
    pool_level = jnp.log((seen_count + 3).astype(jnp.float32))[None, None, :]
    pooled_part = jnp.minimum(pool_level + jax.random.uniform(key_parts[0], (1, HEADS, SEQ), jnp.float32, 0.25, 0.75), 7.0)
    chosen_part = jax.random.uniform(key_parts[1], (1, HEADS, SEQ), jnp.float32, 5.0, 7.0)
    return jnp.concatenate([pooled_part, chosen_part], axis=0).astype(jnp.float32)


def draw_chosen(key, part):
    devices = SEQ // TOK_DEV
    per_device = TOK_DEV // QUERY_BLOCK
    blocks_here = TOK_DEV // KEY_BLOCK
    own_count = QUERY_BLOCK // KEY_BLOCK
    query_blocks = SEQ // QUERY_BLOCK
    free_owners = (CHOSEN - own_count) // 2 - 2
    pair_count = free_owners + 2
    key_parts = jax.random.split(key, 6)
    block_ids = jnp.arange(query_blocks, dtype=jnp.int32)
    device_of = block_ids // per_device
    owner_ids = jnp.arange(devices, dtype=jnp.int32)
    before = (device_of - 1) % devices
    across = (device_of + devices // 2) % devices
    hot_owner = jax.random.randint(key_parts[0], (KV_HEADS, 1, 1), 0, devices)
    owner_score = jax.random.randint(key_parts[1], (KV_HEADS, query_blocks, devices), 0, 1000)
    owner_score = owner_score + jnp.where(owner_ids[None, None, :] == hot_owner, 2000, 0)
    banned = (owner_ids[None, :] == device_of[:, None]) | (owner_ids[None, :] == before[:, None]) | (owner_ids[None, :] == across[:, None])
    owner_score = jnp.where(banned[None], -1, owner_score) * devices + owner_ids[None, None, :]
    _, drawn_owners = lax.top_k(owner_score, free_owners)
    fixed_owners = jnp.broadcast_to(jnp.stack([before, across], axis=-1)[None], (KV_HEADS, query_blocks, 2))
    pair_owners = jnp.concatenate([fixed_owners, drawn_owners.astype(jnp.int32)], axis=-1)
    shape = (KV_HEADS, query_blocks, pair_count)
    first_pick = jnp.minimum(jax.random.randint(key_parts[2], shape, 0, blocks_here), jax.random.randint(key_parts[3], shape, 0, blocks_here))
    second_pick = (first_pick + 1 + jax.random.randint(key_parts[4], shape, 0, blocks_here - 1)) % blocks_here
    others = jnp.concatenate([pair_owners * blocks_here + first_pick, pair_owners * blocks_here + second_pick], axis=-1)
    own_blocks = block_ids[:, None] * own_count + jnp.arange(own_count, dtype=jnp.int32)[None, :]
    own_blocks = jnp.broadcast_to(own_blocks[None], (KV_HEADS, query_blocks, own_count))
    block_lists = jnp.concatenate([own_blocks, others], axis=-1).astype(jnp.int32)
    sort_keys = jax.random.randint(key_parts[5], (KV_HEADS, query_blocks, CHOSEN), 0, 1 << 20) * CHOSEN + jnp.arange(CHOSEN, dtype=jnp.int32)
    reorder = jnp.argsort(sort_keys, axis=-1)
    return jnp.take_along_axis(block_lists, reorder, axis=-1).astype(jnp.int32)


def levels(rng, extent, shards, low, largest):
    def one(dim, blocks):
        steps = jax.random.uniform(jax.random.fold_in(jax.random.fold_in(rng, 6), dim), (blocks,), jnp.float32, low / len(shards), largest / len(shards))
        return jnp.repeat(jnp.exp(steps), extent[dim] // blocks).reshape((-1,) + (1,) * (len(extent) - dim - 1))

    factor_of = one(*shards[0])
    for cut in shards[1:]:
        factor_of = factor_of * one(*cut)
    return factor_of


def scatter_about(key, shape, deviation, reach, cuts=(), held_as=jnp.bfloat16):
    entries = deviation * jax.random.normal(key, shape, jnp.float32)
    if cuts:
        entries = entries * levels(key, shape, cuts, -0.22, 0.18)
    return jnp.clip(entries, -reach, reach).astype(held_as)


def setup_inputs(seed: int = 0) -> dict:
    arg_keys = jax.random.split(jax.random.key(seed), 9)
    return {
        "hidden_rows": scatter_about(arg_keys[0], (SEQ, MODEL), 1.0, 6.0, ((0, 32),)),
        "queries": scatter_about(arg_keys[1], (SEQ, HEADS * HEAD_DIM), 1.0, 6.0, ((0, 8), (1, 4))),
        "key_rows": draw_key_rows(jax.random.fold_in(arg_keys[8], 71), 0),
        "value_rows": draw_value_rows(jax.random.fold_in(arg_keys[8], 71), 0),
        "branch_gates": jnp.clip(0.05 + 0.9 * jax.random.uniform(arg_keys[4], (2, HEADS, SEQ), jnp.float32) ** levels(arg_keys[4], (2, HEADS, SEQ), ((1, 4), (2, 8)), -0.2, 0.2), 0.05, 0.95),
        "log_sums": draw_log_sums(jax.random.fold_in(arg_keys[8], 71), 0),
        "chosen": draw_chosen(jax.random.fold_in(arg_keys[8], 71), 0),
        "out_grad": scatter_about(arg_keys[7], (SEQ, HEADS * HEAD_DIM), 1.0, 6.0, ((0, 8), (1, 4))),
    }


def rounded(value):
    return lax.optimization_barrier(value.astype(jnp.bfloat16)).astype(jnp.float32)


def attend_back(query_rows, key_set, value_set, cotangent, log_sum, visible, score_scale):
    query_wide = query_rows.astype(jnp.float32)
    key_wide = key_set.astype(jnp.float32)
    value_wide = value_set.astype(jnp.float32)
    scores = jnp.einsum('grd,md->grm', query_wide, key_wide) * score_scale
    weights = jnp.where(visible[None], jnp.exp(scores - log_sum[:, :, None]), 0.0)
    weights_low = rounded(weights)
    branch_out = jnp.einsum('grm,md->grd', weights_low, value_wide)
    row_delta = jnp.sum(cotangent * branch_out, axis=-1)
    grad_prob = jnp.einsum('grd,md->grm', cotangent, value_wide)
    dscore = rounded(weights * (grad_prob - row_delta[:, :, None]))
    dquery = jnp.einsum('grm,md->grd', dscore, key_wide) * score_scale
    grad_key = jnp.einsum('grm,grd->md', dscore, query_wide) * score_scale
    grad_value = jnp.einsum('grm,grd->md', weights_low, cotangent)
    return dquery, grad_key, grad_value


def reference(hidden_rows, queries, key_rows, value_rows, branch_gates, log_sums, chosen, out_grad):
    seq_len = queries.shape[0]
    group_size = HEADS // KV_HEADS
    score_scale = HEAD_DIM ** -0.5
    pool_count = seq_len // POOL_BLOCK
    query_blocks = seq_len // QUERY_BLOCK
    positions = jnp.arange(seq_len, dtype=jnp.int32)
    pool_end = jnp.arange(pool_count, dtype=jnp.int32) * POOL_BLOCK + POOL_BLOCK - 1
    pool_visible = pool_end[None, :] <= positions[:, None]
    block_offsets = jnp.arange(KEY_BLOCK, dtype=jnp.int32)
    query_offsets = jnp.arange(QUERY_BLOCK, dtype=jnp.int32)

    def per_head(which_head):
        key_cols = lax.dynamic_slice_in_dim(key_rows, which_head * HEAD_DIM, HEAD_DIM, 1)
        value_cols = lax.dynamic_slice_in_dim(value_rows, which_head * HEAD_DIM, HEAD_DIM, 1)
        first_col = which_head * group_size * HEAD_DIM
        query_cols = lax.dynamic_slice_in_dim(queries, first_col, group_size * HEAD_DIM, 1)
        query_cols = query_cols.reshape(seq_len, group_size, HEAD_DIM).transpose(1, 0, 2)
        grad_cols = lax.dynamic_slice_in_dim(out_grad, first_col, group_size * HEAD_DIM, 1)
        grad_cols = grad_cols.reshape(seq_len, group_size, HEAD_DIM).transpose(1, 0, 2).astype(jnp.float32)
        gate_cols = lax.dynamic_slice_in_dim(branch_gates, which_head * group_size, group_size, 1)
        sum_cols = lax.dynamic_slice_in_dim(log_sums, which_head * group_size, group_size, 1)
        pooled_keys = jnp.mean(key_cols.astype(jnp.float32).reshape(pool_count, POOL_BLOCK, HEAD_DIM), axis=1).astype(jnp.bfloat16)
        pooled_values = jnp.mean(value_cols.astype(jnp.float32).reshape(pool_count, POOL_BLOCK, HEAD_DIM), axis=1).astype(jnp.bfloat16)
        cot_pool = rounded(gate_cols[0][:, :, None] * grad_cols)
        cot_chosen = rounded(gate_cols[1][:, :, None] * grad_cols)
        pool_dquery, pool_dkeys, pool_dvalues = attend_back(query_cols, pooled_keys, pooled_values, cot_pool, sum_cols[0], pool_visible, score_scale)
        head_lists = lax.dynamic_index_in_dim(chosen, which_head, 0, keepdims=False)

        def one_block(totals, block_index):
            key_total, value_total = totals
            picked = lax.dynamic_index_in_dim(head_lists, block_index, 0, keepdims=False)
            key_index = (picked[:, None] * KEY_BLOCK + block_offsets[None, :]).reshape(-1).astype(jnp.int32)
            row_start = (block_index * QUERY_BLOCK).astype(jnp.int32)
            query_part = lax.dynamic_slice_in_dim(query_cols, row_start, QUERY_BLOCK, 1)
            cot_part = lax.dynamic_slice_in_dim(cot_chosen, row_start, QUERY_BLOCK, 1)
            sum_part = lax.dynamic_slice_in_dim(sum_cols[1], row_start, QUERY_BLOCK, 1)
            visible = key_index[None, :] <= (row_start + query_offsets)[:, None]
            dquery, grad_key, grad_value = attend_back(query_part, key_cols[key_index], value_cols[key_index], cot_part, sum_part, visible, score_scale)
            return (key_total.at[key_index].add(grad_key), value_total.at[key_index].add(grad_value)), dquery

        empty_rows = jnp.zeros((seq_len, HEAD_DIM), jnp.float32)
        (pick_dkeys, pick_dvalues), pick_dquery = lax.scan(one_block, (empty_rows, empty_rows), jnp.arange(query_blocks, dtype=jnp.int32))
        pick_dquery = pick_dquery.transpose(1, 0, 2, 3).reshape(group_size, seq_len, HEAD_DIM)
        head_query = (pool_dquery + pick_dquery).astype(jnp.bfloat16).transpose(1, 0, 2).reshape(seq_len, group_size * HEAD_DIM)
        head_key = (pick_dkeys + jnp.repeat(pool_dkeys, POOL_BLOCK, axis=0) / POOL_BLOCK).astype(jnp.bfloat16)
        head_value = (pick_dvalues + jnp.repeat(pool_dvalues, POOL_BLOCK, axis=0) / POOL_BLOCK).astype(jnp.bfloat16)
        return head_query, head_key, head_value

    head_queries, head_keys, head_values = lax.map(per_head, jnp.arange(KV_HEADS, dtype=jnp.int32))
    grad_queries = head_queries.transpose(1, 0, 2).reshape(seq_len, HEADS * HEAD_DIM)
    grad_keys = head_keys.transpose(1, 0, 2).reshape(seq_len, KV_HEADS * HEAD_DIM)
    grad_values = head_values.transpose(1, 0, 2).reshape(seq_len, KV_HEADS * HEAD_DIM)
    grad_weight = jnp.dot(hidden_rows.T, grad_queries, preferred_element_type=jnp.float32)
    return grad_queries, grad_keys, grad_values, grad_weight
```

```python
import functools

import jax
import jax.numpy as jnp
from jax import lax
from jax.experimental import pallas as pl
from jax.experimental.pallas import tpu as pltpu
from jax.sharding import PartitionSpec as P

HEADS = 32
KV_HEADS = 8
HEAD_DIM = 128
QUERY_BLOCK = 128
KEY_BLOCK = 32
POOL_BLOCK = 32
CHOSEN = 16
CAP = 16

F32 = jnp.float32
BF16 = jnp.bfloat16


def dot_nt(a, b):
    return lax.dot_general(a, b, (((1,), (1,)), ((), ())), preferred_element_type=F32)


def dot_nn(a, b):
    return lax.dot_general(a, b, (((1,), (0,)), ((), ())), preferred_element_type=F32)


def branch_back(keys, values, query_stack, cot_stack, log_row, mask, scale):
    scores = dot_nt(keys, query_stack) * scale
    weights = jnp.where(mask, jnp.exp(scores - log_row), 0.0)
    weights_low = weights.astype(BF16)
    grad_prob = dot_nt(values, cot_stack)
    delta = jnp.sum(weights_low.astype(F32) * grad_prob, axis=0, keepdims=True)
    dscore = (weights * (grad_prob - delta)).astype(BF16)
    dquery = dot_nn(keys.T, dscore)
    return dquery, dot_nn(dscore, query_stack) * scale, dot_nn(weights_low, cot_stack)


def attend_kernel(
    group, section, kv_count, scale,
    place_ref, lists_ref, slot_ref, own_ref,
    q_ref, g_ref, gate_ref, log_ref, k_ref, v_ref,
    dq_ref, send_ref, kept_ref,
    pooled_k, pooled_v, pool_dk, pool_dv, kept,
):
    head = pl.program_id(0)
    step = pl.program_id(1)
    pool_count = pooled_k.shape[0]
    tokens = kept_ref.shape[0]
    pool_here = pool_count // kv_count
    chunk = 8 * POOL_BLOCK

    @pl.when(step == 0)
    def _():
        send_ref[...] = jnp.zeros_like(send_ref)
        kept[...] = jnp.zeros_like(kept)
        pool_dk[...] = jnp.zeros_like(pool_dk)
        pool_dv[...] = jnp.zeros_like(pool_dv)
        pick = (
            lax.broadcasted_iota(jnp.int32, (16, 2 * chunk), 1) // POOL_BLOCK
            == lax.broadcasted_iota(jnp.int32, (16, 2 * chunk), 0)
        ).astype(BF16)

        def pool(i, carry):
            rows = pl.ds(pl.multiple_of(i * 2 * chunk, 2 * chunk), 2 * chunk)
            dest = pl.ds(pl.multiple_of(i * 16, 16), 16)
            pooled_k[dest, :] = (dot_nn(pick, k_ref[rows, :]) / POOL_BLOCK).astype(BF16)
            pooled_v[dest, :] = (dot_nn(pick, v_ref[rows, :]) / POOL_BLOCK).astype(BF16)
            return carry

        lax.fori_loop(0, pool_count // 16, pool, 0)

    query_stack = jnp.concatenate(
        [q_ref[:, r * HEAD_DIM : (r + 1) * HEAD_DIM] for r in range(group)], axis=0
    )
    gates = gate_ref[0].T
    grads = [g_ref[:, r * HEAD_DIM : (r + 1) * HEAD_DIM].astype(F32) for r in range(group)]

    def gated(branch):
        cols = [gates[:, branch * group + r : branch * group + r + 1] for r in range(group)]
        return jnp.concatenate([(c * g).astype(BF16) for c, g in zip(cols, grads)], axis=0)

    def log_row(branch):
        return jnp.concatenate(
            [log_ref[0, branch * group + r : branch * group + r + 1, :] for r in range(group)],
            axis=1,
        )

    width = group * QUERY_BLOCK
    first = place_ref[0] * tokens + step * QUERY_BLOCK
    query_pos = first + lax.broadcasted_iota(jnp.int32, (1, width), 1) % QUERY_BLOCK

    pool_end = (
        lax.broadcasted_iota(jnp.int32, (pool_count, width), 0) * POOL_BLOCK + POOL_BLOCK - 1
    )
    dq_pool, dk, dv = branch_back(
        pooled_k[...], pooled_v[...], query_stack, gated(0), log_row(0),
        pool_end <= query_pos, scale,
    )
    pool_dk[...] += dk
    pool_dv[...] += dv

    ids = [lists_ref[head, step * CHOSEN + c] for c in range(CHOSEN)]
    rows = [pl.ds(pl.multiple_of(i * KEY_BLOCK, KEY_BLOCK), KEY_BLOCK) for i in ids]
    keys = jnp.concatenate([k_ref[r, :] for r in rows], axis=0)
    values = jnp.concatenate([v_ref[r, :] for r in rows], axis=0)
    offset = lax.broadcasted_iota(jnp.int32, (KEY_BLOCK, width), 0)
    key_pos = jnp.concatenate([offset + i * KEY_BLOCK for i in ids], axis=0)
    dq_pick, dk, dv = branch_back(
        keys, values, query_stack, gated(1), log_row(1), key_pos <= query_pos, scale
    )
    both = jnp.concatenate([dk, dv], axis=1)
    for c in range(CHOSEN):
        part = both[c * KEY_BLOCK : (c + 1) * KEY_BLOCK]
        slot = pl.multiple_of(slot_ref[head, step * CHOSEN + c], KEY_BLOCK)
        own = pl.multiple_of(own_ref[head, step * CHOSEN + c], KEY_BLOCK)
        send_ref[pl.ds(slot, KEY_BLOCK), :] = part.astype(BF16)
        kept[pl.ds(own, KEY_BLOCK), :] += part

    dq = (dq_pool + dq_pick) * scale
    for r in range(group):
        dq_ref[:, r * HEAD_DIM : (r + 1) * HEAD_DIM] = dq[
            :, r * QUERY_BLOCK : (r + 1) * QUERY_BLOCK
        ].T.astype(BF16)

    @pl.when(step == pl.num_programs(1) - 1)
    def _():
        kept_ref[...] = kept[:tokens, :]
        for owner in range(kv_count):
            at = owner * section + CAP * KEY_BLOCK
            here = slice(owner * pool_here, (owner + 1) * pool_here)
            send_ref[at : at + pool_here, :HEAD_DIM] = pool_dk[here, :].astype(BF16)
            send_ref[at : at + pool_here, HEAD_DIM:] = pool_dv[here, :].astype(BF16)


def settle_kernel(section, kv_count, place_ref, asked_ref, got_ref, kept_ref, gk_ref, gv_ref, acc):
    head = pl.program_id(0)
    tokens = kept_ref.shape[0]
    pool_here = tokens // POOL_BLOCK
    at = CAP * KEY_BLOCK
    pooled = sum(
        got_ref[i * section + at : i * section + at + pool_here, :].astype(F32)
        for i in range(kv_count)
    ) / POOL_BLOCK
    for j in range(pool_here):
        rows = slice(j * POOL_BLOCK, (j + 1) * POOL_BLOCK)
        acc[rows, :] = kept_ref[rows, :] + pooled[j : j + 1, :]

    def source(i, carry):
        other = lax.rem(place_ref[0] + 1 + i, kv_count)
        for c in range(CAP):
            block = asked_ref[head, other * CAP + c]
            rows = pl.ds(pl.multiple_of(block * KEY_BLOCK, KEY_BLOCK), KEY_BLOCK)
            came = pl.ds(pl.multiple_of(other * section + c * KEY_BLOCK, KEY_BLOCK), KEY_BLOCK)
            acc[rows, :] += got_ref[came, :].astype(F32)
        return carry

    lax.fori_loop(0, kv_count - 1, source, 0)
    gk_ref[...] = acc[:, :HEAD_DIM].astype(BF16)
    gv_ref[...] = acc[:, HEAD_DIM:].astype(BF16)


def body(hidden_rows, queries, key_rows, value_rows, branch_gates, log_sums, chosen, out_grad):
    kv_count = lax.axis_size("kv")
    kv_index = lax.axis_index("kv")
    tokens = queries.shape[0]
    kv_local = key_rows.shape[1] // HEAD_DIM
    group = HEADS // KV_HEADS
    scale = HEAD_DIM ** (-0.5)
    seq_len = tokens * kv_count
    steps = tokens // QUERY_BLOCK
    blocks_here = tokens // KEY_BLOCK
    pool_count = seq_len // POOL_BLOCK
    pool_here = tokens // POOL_BLOCK
    request_count = steps * CHOSEN
    section = CAP * KEY_BLOCK + pool_here
    slot_count = kv_count * CAP

    pair_rows = jnp.concatenate([key_rows, value_rows], axis=1)
    every_pair = lax.all_gather(pair_rows, "kv", axis=0, tiled=True)

    lists = chosen.reshape(kv_local, request_count)
    owners = lists // blocks_here
    local_block = lists % blocks_here
    remote = owners != kv_index
    order = jnp.arange(request_count, dtype=jnp.int32)
    rank_in = jnp.sum(
        (
            (owners[:, :, None] == owners[:, None, :]) & (order[None, None, :] < order[None, :, None])
        ).astype(jnp.int32),
        axis=-1,
    )
    slot_index = jnp.where(remote, owners * CAP + rank_in, slot_count)
    wanted = jnp.sum(
        jnp.where(
            slot_index[:, None, :] == jnp.arange(slot_count, dtype=jnp.int32)[None, :, None],
            local_block[:, None, :],
            0,
        ),
        axis=-1,
    )
    asked_for = lax.all_to_all(wanted, "kv", split_axis=1, concat_axis=1, tiled=True)
    slot_row = jnp.where(remote, owners * section + rank_in * KEY_BLOCK, kv_index * section)
    own_row = jnp.where(remote, tokens, local_block * KEY_BLOCK)
    place = kv_index.astype(jnp.int32).reshape(1)

    def per_head(array):
        return (
            array.reshape(2, kv_local, group, tokens)
            .transpose(1, 0, 2, 3)
            .reshape(kv_local, 2 * group, tokens)
        )

    pairs_flops = 2 * kv_local * group * tokens * HEAD_DIM * (pool_count + CHOSEN * KEY_BLOCK) * 5
    wide = 2 * HEAD_DIM
    grad_queries, send, kept = pl.pallas_call(
        functools.partial(attend_kernel, group, section, kv_count, scale),
        grid_spec=pltpu.PrefetchScalarGridSpec(
            num_scalar_prefetch=4,
            grid=(kv_local, steps),
            in_specs=[
                pl.BlockSpec((QUERY_BLOCK, group * HEAD_DIM), lambda h, b, *_: (b, h)),
                pl.BlockSpec((QUERY_BLOCK, group * HEAD_DIM), lambda h, b, *_: (b, h)),
                pl.BlockSpec((1, 2 * group, QUERY_BLOCK), lambda h, b, *_: (h, 0, b)),
                pl.BlockSpec((1, 2 * group, QUERY_BLOCK), lambda h, b, *_: (h, 0, b)),
                pl.BlockSpec((seq_len, HEAD_DIM), lambda h, b, *_: (0, h)),
                pl.BlockSpec((seq_len, HEAD_DIM), lambda h, b, *_: (0, kv_local + h)),
            ],
            out_specs=[
                pl.BlockSpec((QUERY_BLOCK, group * HEAD_DIM), lambda h, b, *_: (b, h)),
                pl.BlockSpec((kv_count * section, wide), lambda h, b, *_: (0, h)),
                pl.BlockSpec((tokens, wide), lambda h, b, *_: (0, h)),
            ],
            scratch_shapes=[
                pltpu.VMEM((pool_count, HEAD_DIM), BF16),
                pltpu.VMEM((pool_count, HEAD_DIM), BF16),
                pltpu.VMEM((pool_count, HEAD_DIM), F32),
                pltpu.VMEM((pool_count, HEAD_DIM), F32),
                pltpu.VMEM((tokens + KEY_BLOCK, wide), F32),
            ],
        ),
        out_shape=[
            jax.ShapeDtypeStruct((tokens, kv_local * group * HEAD_DIM), BF16),
            jax.ShapeDtypeStruct((kv_count * section, kv_local * wide), BF16),
            jax.ShapeDtypeStruct((tokens, kv_local * wide), F32),
        ],
        cost_estimate=pl.CostEstimate(
            flops=pairs_flops, bytes_accessed=24 * 2**20, transcendentals=0
        ),
        name="attend_back",
    )(
        place, lists, slot_row, own_row,
        queries, out_grad, per_head(branch_gates), per_head(log_sums), every_pair, every_pair,
    )

    got = lax.all_to_all(send, "kv", split_axis=0, concat_axis=0, tiled=True)

    hidden_late, _ = lax.optimization_barrier((hidden_rows, every_pair))
    whole_rows = lax.all_gather(hidden_late, "tp", axis=0, tiled=True)
    terms = lax.dot_general(
        whole_rows, grad_queries, (((0,), (0,)), ((), ())), preferred_element_type=F32
    ).astype(BF16)
    grad_weight = lax.psum_scatter(terms, "kv", scatter_dimension=0, tiled=True).astype(F32)

    grad_keys, grad_values = pl.pallas_call(
        functools.partial(settle_kernel, section, kv_count),
        grid_spec=pltpu.PrefetchScalarGridSpec(
            num_scalar_prefetch=2,
            grid=(kv_local,),
            in_specs=[
                pl.BlockSpec((kv_count * section, wide), lambda h, *_: (0, h)),
                pl.BlockSpec((tokens, wide), lambda h, *_: (0, h)),
            ],
            out_specs=[
                pl.BlockSpec((tokens, HEAD_DIM), lambda h, *_: (0, h)),
                pl.BlockSpec((tokens, HEAD_DIM), lambda h, *_: (0, h)),
            ],
            scratch_shapes=[pltpu.VMEM((tokens, wide), F32)],
        ),
        out_shape=[
            jax.ShapeDtypeStruct((tokens, kv_local * HEAD_DIM), BF16),
            jax.ShapeDtypeStruct((tokens, kv_local * HEAD_DIM), BF16),
        ],
        cost_estimate=pl.CostEstimate(
            flops=4 * 2**20, bytes_accessed=8 * 2**20, transcendentals=0
        ),
        name="settle",
    )(place, asked_for, got, kept)
    return (grad_queries, grad_keys, grad_values, grad_weight)


def solution(mesh):
    placed = (
        P(("kv", "tp"), None),
        P("kv", "tp"),
        P("kv", "tp"),
        P("kv", "tp"),
        P(None, "tp", "kv"),
        P(None, "tp", "kv"),
        P("tp", "kv", None),
        P("kv", "tp"),
    )
    return jax.shard_map(
        body,
        mesh=mesh,
        in_specs=placed,
        out_specs=(P("kv", "tp"), P("kv", "tp"), P("kv", "tp"), P("kv", "tp")),
        check_vma=False,
    )
```
